32 devices in a mesh: sp: 8 (over z, x), tp: 4 (over y, core).
Axes of the slice: x: 2, y: 2, z: 4, core: 2. Of those that a mesh axis runs over, the one named last changes fastest.
Arguments:
- inputs: bfloat16 [8192, 2048], P('sp', 'tp'), may hold values from -6 to 6
- w_query: bfloat16 [2048, 2048], P(None, 'tp'), may hold values from -0.125 to 0.125
- w_value: bfloat16 [2048, 2048], P(None, 'tp'), may hold values from -0.125 to 0.125
- w_forget: bfloat16 [2, 2048, 2048], P(None, None, 'tp'), may hold values from -0.125 to 0.125
- w_gate: bfloat16 [2048, 2048], P(None, 'tp'), may hold values from -0.125 to 0.125
- gate_room: float32 [2, 2048], P(None, 'tp'), as said below
- extra_decay: float32 [16, 8192], P('tp', 'sp'), may hold values from -2 to 0
- out_gain: float32 [2048], P('tp'), may hold values from 0.1 to 1.9
- new_inputs: bfloat16 [128, 2048], replicated, may hold values from -6 to 6
Outputs:
- mixed_rows: bfloat16 [8192, 2048], P('sp', 'tp')
- prompt_state_cache: bfloat16 [16, 128, 128], P('tp')
- new_read: bfloat16 [128, 2048], P(None, 'tp')
The draws below stay inside these ranges and needn't reach their ends.
Inputs may be any that keep to these rules, and one draw needn't show every extreme that they name: `gate_room`: each entry lies between 0.5 / 8192 and 0.1.
All inputs are finite; a program needn't handle non-finite values.
Results may differ from the reference program's by a relative error of at most 0.012.
The reference program's roundings to bfloat16 on the way count: a program that leaves them out, or rounds other values in their place, can miss the bound.
Values may be sent and summed in bfloat16 or wider, within the bound.
A program may use at most 128 MiB of HBM per device.

```python
import jax
import jax.numpy as jnp
from jax import lax

D = 2048
HEADS = 16
HD = 128
BLOCK = 128
TOK_DEV = 1024
NEW = 128
LEN = 8192


def draw_inputs(key, part):
    noise_key, offset_key = jax.random.split(key)
    noise_part = jax.random.normal(noise_key, (LEN, D), jnp.float32)
    offset = 0.7 * jax.random.normal(offset_key, (D,), jnp.float32)
    return jnp.clip(noise_part + offset[None, :], -6.0, 6.0).astype(jnp.bfloat16)


def draw_gate_room(key, part):
    pick_key, slow_key, fast_key = jax.random.split(key, 3)
    slow_share = 0.5
    slow_head = jax.random.uniform(pick_key, (2, HEADS, 1), jnp.float32) < slow_share
    slow_value = jnp.exp(jax.random.uniform(slow_key, (2, HEADS, HD), jnp.float32, jnp.log(0.5), jnp.log(2.0))) / LEN
    fast_value = jnp.exp(jax.random.uniform(fast_key, (2, HEADS, HD), jnp.float32, jnp.log(0.03), jnp.log(0.1)))
    return jnp.where(slow_head, slow_value, fast_value).reshape(2, HEADS * HD)


def draw_extra_decay(key, part):
    scale_key, place_key, loss_key = jax.random.split(key, 3)
    low_end = 0.5
    high_end = 2.0
    factor = jnp.exp(jax.random.uniform(scale_key, (HEADS, LEN // TOK_DEV, 1), jnp.float32, jnp.log(low_end), jnp.log(high_end)))
    stable_result = -0.5 / LEN * jnp.broadcast_to(factor, (HEADS, LEN // TOK_DEV, TOK_DEV)).reshape(HEADS, LEN)
    places = jax.random.randint(place_key, (HEADS, 3, 1), 0, LEN)
    loss_values = jnp.log(jax.random.uniform(loss_key, (HEADS, 3, 1), jnp.float32, 0.6, 0.8))
    at_position = jnp.arange(LEN)[None, None, :] == places
    token_groups = jnp.sum(jnp.where(at_position, loss_values, 0.0), axis=1)
    return stable_result + token_groups


def block_scale(rng, shape, pieces, low, high):
    def one(dim, blocks):
        draws = jax.random.uniform(jax.random.fold_in(jax.random.fold_in(rng, 6), dim), (blocks,), jnp.float32, low / len(pieces), high / len(pieces))
        return jnp.repeat(jnp.exp(draws), shape[dim] // blocks).reshape((-1,) + (1,) * (len(shape) - dim - 1))

    loudness = one(*pieces[0])
    for cut in pieces[1:]:
        loudness = loudness * one(*cut)
    return loudness


def noise(stream_key, shape, spread, reach, cuts=(), held_as=jnp.bfloat16):
    entries = jax.random.normal(stream_key, shape, jnp.float32) * spread
    if len(cuts) > 0:
        entries = block_scale(stream_key, shape, cuts, -0.22, 0.18) * entries
    return jnp.clip(entries, min=-reach, max=reach).astype(held_as)


def setup_inputs(seed: int = 0) -> dict:
    key_list = jax.random.split(jax.random.key(seed), 10)
    inputs = draw_inputs(jax.random.fold_in(key_list[9], 71), 0)
    w_query = noise(key_list[1], (D, HEADS * HD), D ** -0.5, 0.125, ((1, 4),))
    w_value = noise(key_list[2], (D, HEADS * HD), D ** -0.5, 0.125, ((1, 4),))
    w_forget = noise(key_list[3], (2, D, HEADS * HD), D ** -0.5, 0.125, ((2, 4),))
    w_gate = noise(key_list[4], (D, HEADS * HD), D ** -0.5, 0.125, ((1, 4),))
    gate_room = draw_gate_room(jax.random.fold_in(key_list[9], 71), 0)
    extra_decay = draw_extra_decay(jax.random.fold_in(key_list[9], 71), 0)
    out_gain = jnp.clip(1.0 + 0.18 * jax.random.normal(key_list[7], (HEADS * HD,), jnp.float32), 0.1, 1.9)
    new_inputs = noise(key_list[8], (NEW, D), 1.0, 6.0)
    return {"inputs": inputs, "w_query": w_query, "w_value": w_value, "w_forget": w_forget, "w_gate": w_gate, "gate_room": gate_room, "extra_decay": extra_decay, "out_gain": out_gain, "new_inputs": new_inputs}


NORM_EPS = 1e-06
TOP_PRECISION = lax.Precision.HIGHEST

def rounded(matrix):
    return lax.optimization_barrier(matrix.astype(jnp.bfloat16)).astype(jnp.float32)

def gate_keys(gate_pre, room_row):
    return room_row * jax.nn.sigmoid(-gate_pre)

def finish(mixture, gain_rows, gate_pre):
    inverse_rms = lax.rsqrt(lax.optimization_barrier(jnp.mean(mixture * mixture, axis=-1, keepdims=True)) + NORM_EPS)
    return (mixture * inverse_rms * gain_rows * jax.nn.silu(gate_pre)).astype(jnp.bfloat16)

def block_states(query_rows, keys_in, values, log_decay, span_len):
    length, head_count, key_width = query_rows.shape
    value_width = values.shape[-1]
    blocks = length // span_len
    q_blocks = query_rows.reshape(blocks, span_len, head_count, key_width)
    k_blocks = keys_in.reshape(blocks, span_len, head_count, key_width)
    v_blocks = values.reshape(blocks, span_len, head_count, value_width)
    within = jnp.cumsum(log_decay.reshape(blocks, span_len, head_count, key_width), axis=1)
    middle = within[:, span_len // 2:span_len // 2 + 1]
    ending = within[:, span_len - 1:span_len]
    q_carried = q_blocks * jnp.exp(within)
    q_inside = q_blocks * jnp.exp(within - middle)
    k_inside = k_blocks * jnp.exp(middle - within)
    k_ending = k_blocks * jnp.exp(ending - within)
    scores = jnp.einsum('nthk,nshk->nhts', q_inside, k_inside, precision=TOP_PRECISION)
    earlier_mask = jnp.arange(span_len)[:, None] >= jnp.arange(span_len)[None, :]
    scores = jnp.where(earlier_mask, scores, 0.0)
    inside = jnp.einsum('nhts,nshv->nthv', scores, v_blocks, precision=TOP_PRECISION)
    additions = jnp.einsum('nshk,nshv->nhkv', k_ending, v_blocks, precision=TOP_PRECISION)
    block_decay = ending[:, 0]

    def advance(current, block_item):
        added_term, decay_sum = block_item
        return (jnp.exp(decay_sum)[:, :, None] * current + added_term, current)
    initial = jnp.zeros((head_count, key_width, value_width), jnp.float32)
    last_state, before = lax.scan(advance, initial, (additions, block_decay))
    carried = jnp.einsum('nthk,nhkv->nthv', q_carried, before, precision=TOP_PRECISION)
    offsets = jnp.cumsum(block_decay, axis=0) - block_decay
    cumulative = (within + offsets[:, None]).reshape(length, head_count, key_width)
    return ((inside + carried).reshape(length, head_count, value_width), last_state, cumulative)

def reference(inputs, w_query, w_value, w_forget, w_gate, gate_room, extra_decay, out_gain, new_inputs):
    head_count = extra_decay.shape[0]
    tokens = inputs.shape[0]
    channels = w_query.shape[1]
    key_width = channels // head_count
    split_heads = (tokens, head_count, key_width)

    def project(matrix_in, weight):
        return jnp.dot(matrix_in, weight, preferred_element_type=jnp.float32)
    query_rows = rounded(project(inputs, w_query)).reshape(split_heads)
    values = rounded(project(inputs, w_value)).reshape(split_heads)
    room_forward = gate_room[0].reshape(head_count, key_width)
    room_backward = gate_room[1].reshape(head_count, key_width)
    gain_rows = out_gain.reshape(head_count, key_width)
    extra_log = extra_decay.T[:, :, None]
    forward_key = gate_keys(project(inputs, w_forget[0]).reshape(split_heads), room_forward)
    backward_key = gate_keys(project(inputs, w_forget[1]).reshape(split_heads), room_backward)
    forward_log = jnp.log1p(-forward_key) + extra_log
    backward_log = jnp.log1p(-backward_key) + extra_log
    forward_out, last_state, unused_sum = block_states(query_rows, forward_key, values, forward_log, BLOCK)
    backward_rev, unused_state, unused_cum = block_states(query_rows[::-1], backward_key[::-1], values[::-1], backward_log[::-1], BLOCK)
    gate_pre = project(inputs, w_gate).reshape(split_heads)
    mixed_rows = finish(forward_out + backward_rev[::-1], gain_rows, gate_pre).reshape(tokens, channels)
    prompt_state_cache = last_state.astype(jnp.bfloat16)
    new_count = new_inputs.shape[0]
    new_heads = (new_count, head_count, key_width)
    fresh_query = rounded(project(new_inputs, w_query)).reshape(new_heads)
    new_value = rounded(project(new_inputs, w_value)).reshape(new_heads)
    fresh_forward = gate_keys(project(new_inputs, w_forget[0]).reshape(new_heads), room_forward)
    new_backward = gate_keys(project(new_inputs, w_forget[1]).reshape(new_heads), room_backward)
    new_gate = project(new_inputs, w_gate).reshape(new_heads)
    cache_entries = jnp.einsum('awe,wel->awl', fresh_query * (1.0 - fresh_forward), prompt_state_cache.astype(jnp.float32), precision=TOP_PRECISION)
    own_term = lax.optimization_barrier(jnp.sum(fresh_query * (fresh_forward + new_backward), axis=-1, keepdims=True)) * new_value
    new_read = finish(cache_entries + own_term, gain_rows, new_gate).reshape(new_count, channels)
    return (mixed_rows, prompt_state_cache, new_read)
```

```python
import functools

import jax
import jax.numpy as jnp
from jax import lax
from jax.experimental import pallas as pl
from jax.experimental.pallas import tpu as pltpu
from jax.sharding import PartitionSpec as P

SPAN = 128
NORM_EPS = 1e-06
F32 = jnp.float32
BF16 = jnp.bfloat16
VMEM_BYTES = 60 * 1024 * 1024


def dot(a, b):
    return jnp.dot(a, b, preferred_element_type=F32)


def dot_nt(a, b):
    return lax.dot_general(a, b, (((1,), (1,)), ((), ())), preferred_element_type=F32)


def dot_tn(a, b):
    return lax.dot_general(a, b, (((0,), (0,)), ((), ())), preferred_element_type=F32)


def split_two(a):
    high = a.astype(BF16)
    return high, (a - high.astype(F32)).astype(BF16)


def gate_keys(pre, room_row):
    return room_row * (1.0 / (1.0 + jnp.exp(pre)))


def silu(pre):
    return pre / (1.0 + jnp.exp(-pre))


def finish(mixture, gate):
    mean = jnp.mean(mixture * mixture, axis=-1, keepdims=True)
    return (mixture * lax.rsqrt(mean + NORM_EPS) * gate).astype(BF16)


def lower_mask():
    return lax.broadcasted_iota(jnp.int32, (SPAN, SPAN), 0) >= lax.broadcasted_iota(
        jnp.int32, (SPAN, SPAN), 1
    )


def upper_mask():
    return lax.broadcasted_iota(jnp.int32, (SPAN, SPAN), 0) <= lax.broadcasted_iota(
        jnp.int32, (SPAN, SPAN), 1
    )


def local_kernel(
    heads, count, pieces, x_ref, wq_ref, wv_ref, wf_ref, wg_ref, room_ref, extra_ref, gain_ref, new_ref,
    mix_ref, qc_ref, gate_ref, before_ref, addb_ref, decay_ref, state_ref, total_ref,
    nq_ref, own_ref, ngate_ref,
    run_f, run_b, cum, full_ref, *sems,
):
    step = pl.program_id(0)
    rows = x_ref.shape[0] // pieces
    begin, advance, end = gather_parts(count, pieces, x_ref, full_ref, *sems)
    key_width = wq_ref.shape[1] // heads

    @pl.when(step == 0)
    def _():
        run_f[...] = jnp.zeros_like(run_f)
        run_b[...] = jnp.zeros_like(run_b)
        cum[...] = jnp.zeros_like(cum)
        begin()

    advance(step)
    x = full_ref[pl.ds(pl.multiple_of(step * rows, rows), rows), :]
    room = room_ref[...]
    value_all = dot(x, wv_ref[...]).astype(BF16)
    key_f = gate_keys(dot(x, wf_ref[0]), room[0:1])
    key_b = gate_keys(dot(x, wf_ref[1]), room[1:2])
    query_all = dot(x, wq_ref[...]).astype(BF16).astype(F32)
    gate_ref[...] = (gain_ref[...] * silu(dot(x, wg_ref[...]))).astype(BF16)
    log_f = jnp.log(1.0 - key_f)
    log_b = jnp.log(1.0 - key_b)
    lower = lower_mask()
    upper = upper_mask()
    lower_ones = jnp.where(lower, 1.0, 0.0)
    upper_ones = jnp.where(upper, 1.0, 0.0)
    lower_two = jnp.concatenate([lower_ones, lower_ones], axis=1).astype(BF16)
    upper_two = jnp.concatenate([upper_ones, upper_ones], axis=1).astype(BF16)
    ones = jnp.ones((2 * SPAN, key_width), BF16)
    half = SPAN // 2
    for block in range(rows // SPAN):
        part = slice(block * SPAN, (block + 1) * SPAN)
        sum_f = dot(lower_two, jnp.concatenate(split_two(log_f[part]), axis=0))
        sum_b = dot(upper_two, jnp.concatenate(split_two(log_b[part]), axis=0))
        for head in range(heads):
            lanes = slice(head * key_width, (head + 1) * key_width)
            extra_high, extra_low = split_two(extra_ref[head : head + 1, part])
            extra_high = extra_high.astype(F32)
            extra_low = extra_low.astype(F32)
            extra_f = dot(
                jnp.concatenate(
                    [lower_ones * extra_high, lower_ones * extra_low], axis=1
                ).astype(BF16),
                ones,
            )
            extra_b = dot(
                jnp.concatenate(
                    [upper_ones * extra_high, upper_ones * extra_low], axis=1
                ).astype(BF16),
                ones,
            )
            within_f = sum_f[:, lanes] + extra_f
            within_b = sum_b[:, lanes] + extra_b
            middle_f = within_f[half : half + 1]
            middle_b = within_b[half - 1 : half]
            ending_f = within_f[SPAN - 1 : SPAN]
            ending_b = within_b[0:1]
            query = query_all[part, lanes]
            values = value_all[part, lanes]
            q_f = query * jnp.exp(within_f - middle_f)
            q_b = query * jnp.exp(within_b - middle_b)
            k_f = key_f[part, lanes] * jnp.exp(middle_f - within_f)
            k_b = key_b[part, lanes] * jnp.exp(middle_b - within_b)
            score_f = dot_nt(q_f.astype(BF16), k_f.astype(BF16))
            score_b = dot_nt(q_b.astype(BF16), k_b.astype(BF16))
            score = jnp.where(lower, score_f, 0.0) + jnp.where(upper, score_b, 0.0)
            mix_ref[part, lanes] = dot(score.astype(BF16), values)
            two = slice(2 * head * key_width, 2 * (head + 1) * key_width)
            qc_ref[part, two] = jnp.concatenate(
                [(q_f * jnp.exp(middle_f)), (q_b * jnp.exp(middle_b))], axis=1
            ).astype(BF16)
            k_end = jnp.concatenate(
                [k_f * jnp.exp(ending_f - middle_f), k_b * jnp.exp(ending_b - middle_b)], axis=1
            ).astype(BF16)
            added = dot_tn(values, k_end)
            add_f = added[:, :key_width]
            add_b = added[:, key_width:]
            before_ref[block, head] = run_f[head]
            addb_ref[block, head] = add_b
            decay_ref[block, 0:1, lanes] = jnp.exp(cum[0:1, lanes])
            decay_ref[block, 1:2, lanes] = jnp.exp(ending_b)
            run_f[head] = jnp.exp(ending_f) * run_f[head] + add_f
            run_b[head] = run_b[head] + jnp.exp(cum[1:2, lanes]) * add_b
            cum[0:1, lanes] = cum[0:1, lanes] + ending_f
            cum[1:2, lanes] = cum[1:2, lanes] + ending_b

    @pl.when(step == pl.num_programs(0) - 1)
    def _():
        end()
        state_ref[0] = run_f[...]
        state_ref[1] = run_b[...]
        total_ref[...] = cum[...]
        new = new_ref[...]
        new_query = dot(new, wq_ref[...]).astype(BF16).astype(F32)
        new_value = dot(new, wv_ref[...]).astype(BF16).astype(F32)
        new_f = gate_keys(dot(new, wf_ref[0]), room[0:1])
        new_b = gate_keys(dot(new, wf_ref[1]), room[1:2])
        ngate_ref[...] = gain_ref[...] * silu(dot(new, wg_ref[...]))
        nq_ref[...] = new_query * (1.0 - new_f)
        both = new_query * (new_f + new_b)
        for head in range(heads):
            lanes = slice(head * key_width, (head + 1) * key_width)
            own_ref[:, lanes] = (
                jnp.sum(both[:, lanes], axis=-1, keepdims=True) * new_value[:, lanes]
            )


def gather_parts(count, pieces, x_ref, full_ref, own_sem, send_sem, recv_sem, pass_sem, come_sem):
    me = lax.axis_index("tp")
    chips = count // 2
    core = lax.rem(me, 2)
    chip = lax.div(me, 2)
    partner = chip * 2 + (1 - core)
    rows = x_ref.shape[0] // pieces
    width = x_ref.shape[1]

    def peer(hop):
        return lax.rem(chip + hop, chips) * 2 + core

    def place(owner, piece):
        return full_ref.at[
            pl.ds(pl.multiple_of(piece * rows, rows), rows), pl.ds(pl.multiple_of(owner * width, width), width)
        ]

    def copy(source, target, sem_out, sem_in, device):
        return pltpu.make_async_remote_copy(
            src_ref=source,
            dst_ref=target,
            send_sem=sem_out,
            recv_sem=sem_in,
            device_id={"tp": device},
            device_id_type=pl.DeviceIdType.MESH,
        )

    own = [x_ref.at[pl.ds(piece * rows, rows)] for piece in range(pieces)]
    keep = pltpu.make_async_copy(
        x_ref, full_ref.at[:, pl.ds(pl.multiple_of(me * width, width), width)], own_sem
    )

    def across(piece, hop):
        return copy(
            own[piece], place(me, piece), send_sem.at[hop, piece], recv_sem.at[hop, piece],
            peer(hop),
        )

    def beside(block, source, hop, piece):
        return copy(source, block, pass_sem.at[hop, piece], come_sem.at[hop, piece], partner)

    def begin():
        barrier = pltpu.get_barrier_semaphore()
        for device in [partner] + [peer(hop) for hop in range(1, chips)]:
            pl.semaphore_signal(
                barrier, inc=1, device_id={"tp": device}, device_id_type=pl.DeviceIdType.MESH
            )
        pl.semaphore_wait(barrier, chips)
        for piece in range(pieces):
            for hop in range(1, chips):
                across(piece, hop).start()
        for piece in range(pieces):
            beside(place(me, piece), own[piece], 0, piece).start()
        keep.start()
        keep.wait()

    def advance(piece):
        for hop in range(1, chips):
            owner = lax.rem(chip + chips - hop, chips) * 2 + core
            block = place(owner, piece)
            copy(
                block, block, send_sem.at[hop, piece], recv_sem.at[hop, piece], peer(hop)
            ).wait_recv()
            beside(block, block, hop, piece).start()
        for hop in range(chips):
            owner = lax.rem(chip + chips - hop, chips) * 2 + (1 - core)
            block = place(owner, piece)
            beside(block, block, hop, piece).wait_recv()

    def end():
        for piece in range(pieces):
            for hop in range(1, chips):
                across(piece, hop).wait_send()
            beside(place(me, piece), own[piece], 0, piece).wait_send()
            for hop in range(1, chips):
                block = place(lax.rem(chip + chips - hop, chips) * 2 + core, piece)
                beside(block, block, hop, piece).wait_send()

    return begin, advance, end


def exchange_kernel(
    count, key_width, state_ref, total_ref, inflow_ref, final_ref,
    got, totals, infl, last,
    own_sem, send_sem, recv_sem, tsend_sem, trecv_sem, isend_sem, irecv_sem, fsend_sem, frecv_sem,
):
    me = lax.axis_index("sp")
    rows = got.shape[2]
    per_head = key_width // rows

    def copy(source, target, sem_out, sem_in, device):
        return pltpu.make_async_remote_copy(
            src_ref=source,
            dst_ref=target,
            send_sem=sem_out,
            recv_sem=sem_in,
            device_id={"sp": device},
            device_id_type=pl.DeviceIdType.MESH,
        )

    def cut(owner):
        return pl.ds(pl.multiple_of(owner * rows, rows), rows)

    def to(hop):
        return lax.rem(me + hop, count)

    def source_of(hop):
        return lax.rem(me + count - hop, count)

    barrier = pltpu.get_barrier_semaphore()
    for hop in range(1, count):
        pl.semaphore_signal(
            barrier, inc=1, device_id={"sp": to(hop)}, device_id_type=pl.DeviceIdType.MESH
        )
    pl.semaphore_wait(barrier, count - 1)
    sent = []
    for hop in range(1, count):
        device = to(hop)
        small = copy(total_ref, totals.at[me], tsend_sem.at[hop], trecv_sem.at[hop], device)
        small.start()
        large = copy(
            state_ref.at[:, cut(device)], got.at[me], send_sem.at[hop], recv_sem.at[hop], device
        )
        large.start()
        sent += [small, large]
    got[me] = state_ref[:, cut(me)]
    totals[me] = total_ref[...]
    for hop in range(1, count):
        source = source_of(hop)
        copy(
            total_ref, totals.at[source], tsend_sem.at[hop], trecv_sem.at[hop], to(hop)
        ).wait_recv()
        copy(
            got.at[source], got.at[source], send_sem.at[hop], recv_sem.at[hop], to(hop)
        ).wait_recv()
    lanes = pl.ds(pl.multiple_of(lax.div(me, per_head) * key_width, key_width), key_width)
    run = jnp.zeros((rows, key_width), F32)
    for source in range(count):
        infl[source, 0] = run
        run = jnp.exp(totals[source, 0:1, lanes]) * run + got[source, 0]
    last[...] = run.astype(last.dtype)
    run = jnp.zeros((rows, key_width), F32)
    for source in reversed(range(count)):
        infl[source, 1] = run
        run = jnp.exp(totals[source, 1:2, lanes]) * run + got[source, 1]
    for hop in range(1, count):
        device = to(hop)
        large = copy(
            infl.at[device], inflow_ref.at[:, cut(me)], isend_sem.at[hop], irecv_sem.at[hop],
            device,
        )
        large.start()
        small = copy(last, final_ref.at[cut(me)], fsend_sem.at[hop], frecv_sem.at[hop], device)
        small.start()
        sent += [large, small]
    keep = [
        pltpu.make_async_copy(infl.at[me], inflow_ref.at[:, cut(me)], own_sem.at[0]),
        pltpu.make_async_copy(last, final_ref.at[cut(me)], own_sem.at[1]),
    ]
    for own in keep:
        own.start()
    for hop in range(1, count):
        source = source_of(hop)
        block = inflow_ref.at[:, cut(source)]
        copy(block, block, isend_sem.at[hop], irecv_sem.at[hop], to(hop)).wait_recv()
        block = final_ref.at[cut(source)]
        copy(block, block, fsend_sem.at[hop], frecv_sem.at[hop], to(hop)).wait_recv()
    for own in keep:
        own.wait()
    for out in sent:
        out.wait_send()


def inflow_kernel(
    heads, inflow_ref, final_ref, mix_ref, qc_ref, gate_ref, before_ref, addb_ref, decay_ref,
    nq_ref, own_ref, ngate_ref,
    out_ref, cache_ref, read_ref,
    in_b,
):
    step = pl.program_id(0)
    rows = mix_ref.shape[0]
    key_width = mix_ref.shape[1] // heads

    @pl.when(step == 0)
    def _():
        in_b[...] = inflow_ref[1]
        for head in range(heads):
            lanes = slice(head * key_width, (head + 1) * key_width)
            final = final_ref[head].astype(F32)
            cache_ref[head] = final.T.astype(BF16)
            rounded = final.astype(BF16)
            mixture = own_ref[:, lanes] + dot_nt(
                jnp.concatenate(split_two(nq_ref[:, lanes]), axis=1),
                jnp.concatenate([rounded, rounded], axis=1),
            )
            read_ref[:, lanes] = finish(mixture, ngate_ref[:, lanes])

    for block in reversed(range(rows // SPAN)):
        part = slice(block * SPAN, (block + 1) * SPAN)
        for head in range(heads):
            lanes = slice(head * key_width, (head + 1) * key_width)
            two = slice(2 * head * key_width, 2 * (head + 1) * key_width)
            state_f = before_ref[block, head] + decay_ref[block, 0:1, lanes] * inflow_ref[0, head]
            state_b = in_b[head]
            high, low = split_two(jnp.concatenate([state_f, state_b], axis=1))
            q_two = qc_ref[part, two]
            mixture = mix_ref[part, lanes] + dot_nt(
                jnp.concatenate([q_two, q_two], axis=1), jnp.concatenate([high, low], axis=1)
            )
            out_ref[part, lanes] = finish(mixture, gate_ref[part, lanes].astype(F32))
            in_b[head] = decay_ref[block, 1:2, lanes] * state_b + addb_ref[block, head]


def per_device(
    inputs, w_query, w_value, w_forget, w_gate, gate_room, extra_decay, out_gain, new_inputs
):
    heads = extra_decay.shape[0]
    tokens = inputs.shape[0]
    channels = w_query.shape[1]
    width = w_query.shape[0]
    key_width = channels // heads
    new_count = new_inputs.shape[0]
    blocks = tokens // SPAN
    chunk_blocks = 2 if blocks % 2 == 0 else 1
    chunk = chunk_blocks * SPAN
    steps = tokens // chunk
    parts = width // inputs.shape[1]
    dma = pltpu.SemaphoreType.DMA
    def whole(shape):
        return pl.BlockSpec(shape, lambda i: (0,) * len(shape), pipeline_mode=pl.Buffered(1))

    def kept(shape):
        return pl.BlockSpec(shape, lambda i: (0,) * len(shape))

    def by_rows(shape):
        return pl.BlockSpec(shape, lambda i: (i,) + (0,) * (len(shape) - 1))

    def reverse_rows(shape):
        return pl.BlockSpec(shape, lambda i: (steps - 1 - i,) + (0,) * (len(shape) - 1))

    shapes = [
        ((tokens, channels), F32, (chunk, channels)),
        ((tokens, 2 * channels), BF16, (chunk, 2 * channels)),
        ((tokens, channels), BF16, (chunk, channels)),
        ((blocks, heads, key_width, key_width), F32, (chunk_blocks, heads, key_width, key_width)),
        ((blocks, heads, key_width, key_width), F32, (chunk_blocks, heads, key_width, key_width)),
        ((blocks, 2, channels), F32, (chunk_blocks, 2, channels)),
    ]
    finals = [
        ((2, heads, key_width, key_width), F32),
        ((2, channels), F32),
        ((new_count, channels), F32),
        ((new_count, channels), F32),
        ((new_count, channels), F32),
    ]
    mix, carried, gate, before, add_b, decay, state, total, new_q, own, new_gate = pl.pallas_call(
        functools.partial(local_kernel, heads, parts, steps),
        grid=(steps,),
        out_shape=[jax.ShapeDtypeStruct(s, d) for s, d, _ in shapes]
        + [jax.ShapeDtypeStruct(s, d) for s, d in finals],
        in_specs=[
            whole((tokens, width // parts)),
            whole((width, channels)),
            whole((width, channels)),
            whole((2, width, channels)),
            whole((width, channels)),
            whole((2, channels)),
            pl.BlockSpec((heads, chunk), lambda i: (0, i)),
            whole((1, channels)),
            whole((new_count, width)),
        ],
        out_specs=[by_rows(b) for _, _, b in shapes] + [kept(s) for s, _ in finals],
        scratch_shapes=[
            pltpu.VMEM((heads, key_width, key_width), F32),
            pltpu.VMEM((heads, key_width, key_width), F32),
            pltpu.VMEM((2, channels), F32),
            pltpu.VMEM((tokens, width), BF16),
            dma,
        ]
        + [dma((parts // 2, steps))] * 4,
        compiler_params=pltpu.CompilerParams(
            collective_id=0, has_side_effects=True,
            dimension_semantics=("arbitrary",), vmem_limit_bytes=VMEM_BYTES
        ),
        name="local",
    )(inputs, w_query, w_value, w_forget, w_gate, gate_room, extra_decay, out_gain[None], new_inputs)
    count = lax.axis_size("sp")
    cut_rows = channels // count
    final_type = BF16 if cut_rows % 16 == 0 else F32
    inflow, final = pl.pallas_call(
        functools.partial(exchange_kernel, count, key_width),
        out_shape=[
            jax.ShapeDtypeStruct((2, channels, key_width), F32),
            jax.ShapeDtypeStruct((channels, key_width), final_type),
        ],
        in_specs=[pl.BlockSpec(memory_space=pltpu.VMEM)] * 2,
        out_specs=[pl.BlockSpec(memory_space=pl.ANY)] * 2,
        scratch_shapes=[
            pltpu.VMEM((count, 2, cut_rows, key_width), F32),
            pltpu.VMEM((count, 2, channels), F32),
            pltpu.VMEM((count, 2, cut_rows, key_width), F32),
            pltpu.VMEM((cut_rows, key_width), final_type),
            dma((2,)),
        ]
        + [dma((count,))] * 8,
        compiler_params=pltpu.CompilerParams(collective_id=1, has_side_effects=True),
        name="exchange",
    )(state.reshape(2, channels, key_width), total)
    inflow = inflow.reshape(2, heads, key_width, key_width)
    final = final.reshape(heads, key_width, key_width)
    return tuple(
        pl.pallas_call(
            functools.partial(inflow_kernel, heads),
            grid=(steps,),
            out_shape=[
                jax.ShapeDtypeStruct((tokens, channels), BF16),
                jax.ShapeDtypeStruct((heads, key_width, key_width), BF16),
                jax.ShapeDtypeStruct((new_count, channels), BF16),
            ],
            in_specs=[
                whole((2, heads, key_width, key_width)),
                whole((heads, key_width, key_width)),
            ]
            + [reverse_rows(b) for _, _, b in shapes]
            + [whole(s) for s, _ in finals[2:]],
            out_specs=[
                reverse_rows((chunk, channels)),
                kept((heads, key_width, key_width)),
                kept((new_count, channels)),
            ],
            scratch_shapes=[pltpu.VMEM((heads, key_width, key_width), F32)],
            compiler_params=pltpu.CompilerParams(
                dimension_semantics=("arbitrary",), vmem_limit_bytes=VMEM_BYTES
            ),
            name="inflow",
        )(inflow, final, mix, carried, gate, before, add_b, decay, new_q, own, new_gate)
    )


def solution(mesh):
    return jax.shard_map(
        per_device,
        mesh=mesh,
        in_specs=(
            P("sp", "tp"),
            P(None, "tp"),
            P(None, "tp"),
            P(None, None, "tp"),
            P(None, "tp"),
            P(None, "tp"),
            P("tp", "sp"),
            P("tp"),
            P(),
        ),
        out_specs=(P("sp", "tp"), P("tp", None, None), P(None, "tp")),
        check_vma=False,
    )
```
